1024 devices in a mesh: rep: 2 (over z_hi), fs: 64 (over z_lo, y), tp: 8 (over x, core).
Axes of the slice: x: 4, y: 8, z: 16 (z_hi: 2, z_lo: 8; z = z_hi * 8 + z_lo), core: 2. Of those that a mesh axis runs over, the one named last changes fastest.
Arguments:
- activations: bfloat16 [2048, 65536], P(None, ('rep', 'fs')), may hold values from -60 to 60
- w_mix_in: bfloat16 [2048, 1024], P('fs', 'tp'), may hold values from -0.125 to 0.125
- w_mix_out: bfloat16 [2048, 1024], P('fs', 'tp'), may hold values from -0.1875 to 0.1875
- w_gate: bfloat16 [2048, 2816], P('fs', 'tp'), may hold values from -0.125 to 0.125
- w_up: bfloat16 [2048, 2816], P('fs', 'tp'), may hold values from -0.125 to 0.125
- w_down: bfloat16 [2048, 2816], P('fs', 'tp'), may hold values from -0.109375 to 0.109375
- pool_scale: float32 [1024], replicated, may hold values from 0.1 to 1.9
- gain_mix: float32 [2048], replicated, may hold values from 0.1 to 1.9
- gain_ffn: float32 [2048], replicated, may hold values from 0.1 to 1.9
- gain_out: float32 [2048], replicated, may hold values from 0.1 to 1.9
Outputs:
- normalized: bfloat16 [2048, 65536], P('tp', ('rep', 'fs'))
The draws below stay inside these ranges and needn't reach their ends.
All inputs are finite; a program needn't handle non-finite values.
Results may differ from the reference program's by a relative error of at most 0.014.
Values may be sent and summed in bfloat16 or wider, within the bound.
A program may use at most 64 MiB of HBM per device.

```python
import jax
import jax.numpy as jnp
from jax import lax

D = 2048
BRANCH = 1024
FF = 2816
POOL_GROUP = 256
SEQ_LEN = 256
TOKENS = 65536
N_TP = 8


def draw_activations(key, part):
    key_rough, key_noise = jax.random.split(key, 2)
    feature_place = jnp.arange(D, dtype=jnp.float32)[:, None] / D
    rough = jax.random.uniform(key_rough, (D, 1), jnp.float32, -0.3, 0.3)
    feature_scale = 0.5 * jnp.exp(jnp.log(8.0) * feature_place + rough)
    values = jnp.clip(jax.random.normal(key_noise, (D, TOKENS), jnp.float32), -6.0, 6.0)
    return jnp.clip(values * feature_scale, -60.0, 60.0).astype(jnp.bfloat16)


def levels(own_key, shape, shards, smallest, top_value):
    def one(axis_at, blocks):
        draws = jax.random.uniform(jax.random.fold_in(jax.random.fold_in(own_key, 6), axis_at), (blocks,), jnp.float32, smallest / len(shards), top_value / len(shards))
        return jnp.repeat(jnp.exp(draws), shape[axis_at] // blocks).reshape((-1,) + (1,) * (len(shape) - axis_at - 1))

    gain = one(*shards[0])
    for cut in shards[1:]:
        gain = gain * one(*cut)
    return gain


def gaussian(rng, shape, scale, reach, shards=(), kind=jnp.bfloat16):
    drawn = scale * jax.random.normal(rng, shape, jnp.float32)
    if shards:
        drawn = drawn * levels(rng, shape, shards, -0.22, 0.18)
    return jnp.clip(drawn, -reach, reach).astype(kind)


def setup_inputs(seed: int = 0) -> dict:
    key_list = jax.random.split(jax.random.key(seed), 11)
    activations = draw_activations(jax.random.fold_in(key_list[10], 71), 0)
    w_mix_in = gaussian(key_list[1], (D, BRANCH), D ** -0.5, 0.125, ((0, 64), (1, 8)))
    w_mix_out = gaussian(key_list[2], (D, BRANCH), BRANCH ** -0.5, 0.1875, ((0, 64), (1, 8)))
    w_gate = gaussian(key_list[3], (D, FF), D ** -0.5, 0.125, ((0, 64), (1, 8)))
    w_up = gaussian(key_list[4], (D, FF), D ** -0.5, 0.125, ((0, 64), (1, 8)))
    w_down = gaussian(key_list[5], (D, FF), FF ** -0.5, 0.109375, ((0, 64), (1, 8)))
    pool_scale = jnp.clip(1.0 + 0.18 * jax.random.normal(key_list[6], (BRANCH,), jnp.float32), 0.1, 1.9)
    gain_mix = jnp.clip(1.0 + 0.18 * jax.random.normal(key_list[7], (D,), jnp.float32), 0.1, 1.9)
    gain_ffn = jnp.clip(1.0 + 0.18 * jax.random.normal(key_list[8], (D,), jnp.float32), 0.1, 1.9)
    gain_out = jnp.clip(1.0 + 0.18 * jax.random.normal(key_list[9], (D,), jnp.float32), 0.1, 1.9)
    return {"activations": activations, "w_mix_in": w_mix_in, "w_mix_out": w_mix_out, "w_gate": w_gate, "w_up": w_up, "w_down": w_down, "pool_scale": pool_scale, "gain_mix": gain_mix, "gain_ffn": gain_ffn, "gain_out": gain_out}


EPS = 1e-06
WINDOWS = (2, 4, 8, 16)

def rms_factor(stream):
    return lax.rsqrt(lax.optimization_barrier(jnp.mean(stream * stream, axis=0, keepdims=True)) + EPS)

def pool_tokens(inputs, group_of):
    channels = inputs.shape[0]
    values = inputs.astype(jnp.float32).reshape(channels, -1, SEQ_LEN)
    sequences = values.shape[1]
    running = jnp.concatenate([jnp.zeros((channels, sequences, 1), jnp.float32), jnp.cumsum(values, axis=-1)], axis=-1)
    places = jnp.arange(SEQ_LEN, dtype=jnp.int32)
    pooled_sum = jnp.zeros_like(values)
    for group_id, window in enumerate(WINDOWS):
        behind = window // 2
        onward = window - behind
        upper_sum = jnp.concatenate([running, jnp.repeat(running[..., -1:], onward, axis=-1)], axis=-1)[..., onward:onward + SEQ_LEN]
        lower_sum = jnp.concatenate([jnp.zeros((channels, sequences, behind), jnp.float32), running], axis=-1)[..., :SEQ_LEN]
        counts = (jnp.minimum(places + onward, SEQ_LEN) - jnp.maximum(places - behind, 0)).astype(jnp.float32)
        window_mean = (upper_sum - lower_sum) / counts
        pooled_sum = pooled_sum + jnp.where((group_of == group_id)[:, None, None], window_mean, 0.0)
    return (pooled_sum - values).reshape(channels, -1)

def block_sum(weights, acts, blocks):
    width = acts.shape[0] // blocks
    stacked_weights = jnp.transpose(weights.reshape(weights.shape[0], blocks, width), (1, 0, 2))
    stacked_acts = acts.reshape(blocks, width, acts.shape[1])

    def add_block(carry, pair):
        term = jnp.dot(pair[0], pair[1], preferred_element_type=jnp.float32).astype(jnp.bfloat16)
        term = lax.optimization_barrier(term)
        return (carry + term.astype(jnp.float32), None)
    start = jnp.zeros((weights.shape[0], acts.shape[1]), jnp.float32)
    total, _ = lax.scan(add_block, start, (stacked_weights, stacked_acts))
    return total

def reference(activations, w_mix_in, w_mix_out, w_gate, w_up, w_down, pool_scale, gain_mix, gain_ffn, gain_out):
    stream = activations.astype(jnp.float32)
    normed = (stream * rms_factor(stream) * gain_mix[:, None]).astype(jnp.bfloat16)
    inputs = jnp.dot(w_mix_in.T, normed, preferred_element_type=jnp.float32).astype(jnp.bfloat16)
    group_of = (jnp.arange(BRANCH, dtype=jnp.int32) // POOL_GROUP).astype(jnp.int32)
    pooled = (pool_tokens(inputs, group_of) * pool_scale[:, None]).astype(jnp.bfloat16)
    mixed = block_sum(w_mix_out, pooled, N_TP)
    after_mix = lax.optimization_barrier((stream + mixed).astype(jnp.bfloat16)).astype(jnp.float32)
    normed_two = (after_mix * rms_factor(after_mix) * gain_ffn[:, None]).astype(jnp.bfloat16)
    gate = jnp.dot(w_gate.T, normed_two, preferred_element_type=jnp.float32)
    upward = jnp.dot(w_up.T, normed_two, preferred_element_type=jnp.float32)
    hidden = (jax.nn.silu(gate) * upward).astype(jnp.bfloat16)
    ffn_out = block_sum(w_down, hidden, N_TP)
    final = after_mix + ffn_out
    return (final * rms_factor(final) * gain_out[:, None]).astype(jnp.bfloat16)
```

```python
import jax
import jax.numpy as jnp
from jax import lax
from jax.experimental import pallas as pl
from jax.experimental.pallas import tpu as pltpu
from jax.sharding import PartitionSpec as P

F32 = jnp.float32
BF16 = jnp.bfloat16
SEQ = 256
EPS = 1e-06
TOK = 512
D = 2048
HID = 384
MESH = pl.DeviceIdType.MESH
MIX_IN, MIX_OUT, GATE, UP, DOWN = range(5)
HALVES = (1, 2, 1, 1, 2)


def wide(tile, times):
    return jnp.concatenate([tile] * times, axis=1)


def spread_row(row):
    return jnp.transpose(jnp.broadcast_to(row, (128, 128)))


def dot(a, b):
    return jnp.dot(a, b, preferred_element_type=F32)


def dot_first(a, b):
    return lax.dot_general(a, b, (((0,), (0,)), ((), ())), preferred_element_type=F32)


def kernel(
    x_hbm, wi_hbm, wo_hbm, wf_hbm, scale_ref, g1_ref, g2_ref, g3_ref,
    out_ref,
    xb, hb, x1b, mb, ob, opb, gb, ub, db, pc, pp, gcol, hid,
    to_pair, from_pair, own, far2, rgt, lft, keep_r, keep_l, in_l, in_r, in_far, ssq,
    loc_sem, p1_send, p1_recv, p2_send, p2_recv, xo_send, xo_recv, d2_send, d2_recv,
    p_send, p_recv, rs_send, rs_recv, q_send, q_recv,
):
    rep, fs, tp = lax.axis_index("rep"), lax.axis_index("fs"), lax.axis_index("tp")
    zl, y = fs // 8, fs % 8
    z = rep * 8 + zl
    x, c = tp // 2, tp % 2
    a_own = y + c * (zl - y)
    b_own = zl + c * (y - zl)

    def device(zz, yy, xx, cc):
        zz = (zz + 32) % 16
        yy = (yy + 16) % 8
        return (zz // 8, (zz % 8) * 8 + yy, ((xx + 8) % 4) * 2 + cc)

    def ring_a(d):
        return device(z + c * d, y + (1 - c) * d, x, c)

    def ring_b(d):
        return device(z + (1 - c) * d, y + c * d, x, c)

    def fidx(b, a):
        return (b * 8 + a) + c * ((a * 8 + b) - (b * 8 + a))

    started = []

    def remote(src, dst, send, recv, dev):
        return pltpu.make_async_remote_copy(
            src_ref=src, dst_ref=dst, send_sem=send, recv_sem=recv, device_id=dev, device_id_type=MESH
        )

    def go(copy):
        copy.start()
        started.append(copy)

    bufs = (mb, ob, gb, ub, db)

    locals_ = [
        pltpu.make_async_copy(wi_hbm, mb.at[b_own, a_own], loc_sem.at[0]),
        pltpu.make_async_copy(
            wo_hbm, ob.at[b_own, a_own, :, pl.ds(pl.multiple_of(x * 128, 128), 128)], loc_sem.at[1]
        ),
        pltpu.make_async_copy(wf_hbm.at[0], gb.at[b_own, a_own], loc_sem.at[2]),
        pltpu.make_async_copy(wf_hbm.at[1], ub.at[b_own, a_own], loc_sem.at[3]),
        pltpu.make_async_copy(wf_hbm.at[2], db.at[b_own, a_own], loc_sem.at[4]),
    ]
    x_copy = pltpu.make_async_copy(x_hbm, xb, loc_sem.at[5])
    for cp in locals_:
        cp.start()
    x_copy.start()
    barrier = pltpu.get_barrier_semaphore()
    peers = [ring_a(d) for d in (1, -1, 2, -2, 3, -3, 4, -4)] + [ring_b(1), ring_b(-1)]
    peers += [device(z, y, x + dx, cc) for dx in (1, 2, 3) for cc in (c, 1 - c)]
    peers += [device(z, y, x, 1 - c)]
    for dev in peers:
        pl.semaphore_signal(barrier, inc=1, device_id=dev, device_id_type=MESH)
    for cp in locals_:
        cp.wait()
    pl.semaphore_wait(barrier, len(peers))

    offsets = (1, -1, 2, -2, 3, -3, 4)

    def p1(t, i):
        blk = bufs[t].at[b_own, a_own]
        return remote(blk, blk, p1_send.at[t, i], p1_recv.at[t, i], ring_a(offsets[i]))

    def p1_start(t):
        for i in range(7):
            go(p1(t, i))

    def p1_wait(t):
        for i in range(7):
            src = (a_own - offsets[i] + 8) % 8
            blk = bufs[t].at[b_own, src]
            remote(blk, blk, p1_send.at[t, i], p1_recv.at[t, i], ring_a(0 - offsets[i])).wait_recv()

    p1_start(MIX_IN)
    wo_dst = ob.at[b_own, a_own, :, pl.ds(pl.multiple_of(x * 128, 128), 128)]
    for dx in (1, 3, 2):
        go(remote(wo_dst, wo_dst, xo_send.at[dx - 1], xo_recv.at[dx - 1], device(z, y, x + dx, c)))
    p1_start(GATE)

    def spread_gain(g_ref):
        for r in range(16):
            gcol[4 * r : 4 * r + 4] = spread_row(g_ref[r : r + 1, :]).reshape(4, 32, 128)

    def add_squares(acc, v):
        return acc + (v * v).reshape(4, 8, TOK).sum(axis=0)

    def factor(acc):
        return lax.rsqrt(jnp.sum(acc, axis=0, keepdims=True) / D + EPS)

    x_copy.wait()
    spread_gain(g1_ref)
    acc1 = lax.fori_loop(
        0, 64, lambda i, acc: add_squares(acc, xb[i].astype(F32)), jnp.zeros((8, TOK), F32)
    )
    r1 = factor(acc1)

    for dx in (1, 3, 2):
        xs = (x - dx + 4) % 4
        got = ob.at[b_own, a_own, :, pl.ds(pl.multiple_of(xs * 128, 128), 128)]
        remote(got, got, xo_send.at[dx - 1], xo_recv.at[dx - 1], device(z, y, x, c)).wait_recv()
    p1_start(MIX_OUT)
    p1_start(UP)
    p1_start(DOWN)

    def row_part(t, row, d, way, half):
        if d == 3:
            return bufs[t].at[row, pl.ds(0, 4)] if way == 1 else bufs[t].at[row, pl.ds(4, 4)]
        if HALVES[t] == 2:
            return bufs[t].at[row, pl.ds(4 * half, 4)]
        return bufs[t].at[row]

    def p2(t, d, way, half, arriving):
        w = (1 - way) // 2
        row = (b_own - way * (d + arriving) + 16) % 8
        part = row_part(t, row, d, way, half)
        at = d * 2 + half
        return remote(part, part, p2_send.at[t, w, at], p2_recv.at[t, w, at], ring_b(way))

    def parts_of(t, d):
        return range(1 if d == 3 else HALVES[t])

    def forward(t, d, half=0):
        for way in (1, -1):
            if d in (1, 2):
                p2(t, d - 1, way, half, 1).wait_recv()
            elif d == 3:
                own_half = 0 if way == 1 else 1
                if HALVES[t] == 2:
                    p2(t, 2, way, own_half, 1).wait_recv()
                else:
                    p2(t, 2, way, 0, 1).wait_recv()
            go(p2(t, d, way, half, 0))
        if d == 3 and HALVES[t] == 2:
            for way in (1, -1):
                other_half = 1 if way == 1 else 0
                p2(t, 2, way, other_half, 1).wait_recv()

    def last(t):
        for way in (1, -1):
            p2(t, 3, way, 0, 1).wait_recv()

    pair = device(z, y, x, 1 - c)

    def to_pair_row(k):
        row = (b_own - k + 16) % 8
        return remote(ob.at[row], opb.at[:, row], d2_send.at[k], d2_recv.at[k], pair)

    p1_wait(MIX_IN)
    forward(MIX_IN, 0)
    p1_wait(MIX_OUT)
    forward(MIX_OUT, 0, 0)

    def scale_h(src, fac):
        def body(i, carry):
            v = src[i].astype(F32) * fac * wide(gcol[i], 4)
            b, a = i // 8, i % 8
            hb[fidx(b, a)] = v.astype(BF16)
            return carry

        lax.fori_loop(0, 64, body, 0)

    scale_h(xb, r1)
    forward(MIX_IN, 1)
    forward(MIX_OUT, 0, 1)
    go(to_pair_row(0))
    forward(MIX_IN, 2)
    p1_wait(GATE)
    forward(GATE, 0)
    forward(MIX_IN, 3)
    forward(MIX_OUT, 1, 0)
    forward(MIX_OUT, 1, 1)
    go(to_pair_row(1))
    go(to_pair_row(7))
    spread_gain(g2_ref)
    last(MIX_IN)

    u = dot_first(mb[...].reshape(D, 128), hb[...].reshape(D, TOK)).astype(BF16)
    behind = lax.shift_left(jnp.int32(1), x.astype(jnp.int32))
    src_place = lax.broadcasted_iota(jnp.int32, (SEQ, SEQ), 0)
    dst_place = lax.broadcasted_iota(jnp.int32, (SEQ, SEQ), 1)
    inside = (src_place >= dst_place - behind) & (src_place < dst_place + behind)
    band = jnp.where(inside, 1.0, 0.0).astype(BF16)
    place = lax.broadcasted_iota(jnp.int32, (1, SEQ), 1)
    counts = (jnp.minimum(place + behind, SEQ) - jnp.maximum(place - behind, 0)).astype(F32)
    scale_col = wide(spread_row(scale_ref[pl.ds(tp, 1), :]), 2)
    for s in range(2):
        us = u[:, s * SEQ : (s + 1) * SEQ]
        mean = dot(us, band) / counts
        pc[x, :, s * SEQ : (s + 1) * SEQ] = ((mean - us.astype(F32)) * scale_col).astype(BF16)

    right, left = device(z, y, x + 1, c), device(z, y, x - 1, c)
    xr, xl, xo = (x + 1) % 4, (x + 3) % 4, (x + 2) % 4
    p1_wait(UP)
    forward(UP, 0)
    go(remote(pc.at[x], pc.at[x], p_send.at[0], p_recv.at[0], right))
    go(remote(pc.at[x], pc.at[x], p_send.at[1], p_recv.at[1], left))
    go(remote(pc.at[x], pp.at[x], p_send.at[2], p_recv.at[2], pair))
    forward(MIX_OUT, 2, 0)
    forward(MIX_OUT, 2, 1)
    go(to_pair_row(2))
    go(to_pair_row(6))
    forward(GATE, 1)
    remote(pc.at[xl], pc.at[xl], p_send.at[0], p_recv.at[0], right).wait_recv()
    lo, hi = pl.ds(0, 64), pl.ds(64, 64)
    go(remote(pc.at[xl, lo], pc.at[xl, lo], p_send.at[3], p_recv.at[3], right))
    go(remote(pc.at[xl], pp.at[xl], p_send.at[4], p_recv.at[4], pair))
    remote(pc.at[xr], pc.at[xr], p_send.at[1], p_recv.at[1], left).wait_recv()
    go(remote(pc.at[xr, hi], pc.at[xr, hi], p_send.at[5], p_recv.at[5], left))
    go(remote(pc.at[xr], pp.at[xr], p_send.at[6], p_recv.at[6], pair))
    forward(MIX_OUT, 3)
    go(to_pair_row(3))
    go(to_pair_row(5))
    forward(UP, 1)
    p1_wait(DOWN)
    remote(pc.at[xo, lo], pc.at[xo, lo], p_send.at[3], p_recv.at[3], right).wait_recv()
    remote(pc.at[xo, hi], pc.at[xo, hi], p_send.at[5], p_recv.at[5], left).wait_recv()
    go(remote(pc.at[xo], pp.at[xo], p_send.at[7], p_recv.at[7], pair))
    forward(GATE, 2)
    last(MIX_OUT)
    go(to_pair_row(4))
    forward(UP, 2)
    forward(DOWN, 0, 0)
    forward(DOWN, 0, 1)
    for n, at in ((2, x), (4, xl), (6, xr), (7, xo)):
        remote(pc.at[at], pp.at[at], p_send.at[n], p_recv.at[n], pair).wait_recv()
    for k in range(8):
        row = (a_own - k + 16) % 8
        remote(ob.at[row], opb.at[:, row], d2_send.at[k], d2_recv.at[k], pair).wait_recv()

    def mix_row(b, acc):
        m = dot(ob[b].reshape(256, 512), pc[...].reshape(512, TOK))
        m = m + dot(opb[b].reshape(256, 512), pp[...].reshape(512, TOK))
        for a in range(8):
            f = fidx(b, a)
            v = (xb[f].astype(F32) + m[a * 32 : (a + 1) * 32]).astype(BF16)
            x1b[f] = v
            acc = add_squares(acc, v.astype(F32))
        return acc

    acc2 = lax.fori_loop(0, 8, mix_row, jnp.zeros((8, TOK), F32))
    forward(GATE, 3)
    forward(UP, 3)
    forward(DOWN, 1, 0)
    forward(DOWN, 1, 1)
    scale_h(x1b, factor(acc2))
    forward(DOWN, 2, 0)
    forward(DOWN, 2, 1)
    last(GATE)
    last(UP)
    forward(DOWN, 3)

    def hidden_half(n, carry):
        at = pl.ds(pl.multiple_of(n * 256, 256), 256)
        rhs = hb[:, :, at].reshape(D, 256)
        g = dot_first(gb[...].reshape(D, HID), rhs)
        v = dot_first(ub[...].reshape(D, HID), rhs)
        hid[:, at] = (g / (1.0 + jnp.exp(-g)) * v).astype(BF16)
        return carry

    lax.fori_loop(0, 2, hidden_half, 0)
    last(DOWN)

    def term(xd, cd):
        t = xd * 2 + cd
        rows = [db[t + c * (i - t), i + c * (t - i)] for i in range(8)]
        return dot(jnp.concatenate(rows, axis=0), hid[...])

    def pair_copy(j):
        return remote(to_pair.at[j], from_pair.at[j], rs_send.at[j], rs_recv.at[j], pair)

    dests = (xo, xr, xl, x)
    to_pair[0] = term(xo, 1 - c).astype(BF16)
    to_pair[1] = term(xr, 1 - c).astype(BF16)
    go(pair_copy(0))
    to_pair[2] = term(xl, 1 - c).astype(BF16)
    go(pair_copy(1))
    to_pair[3] = term(x, 1 - c).astype(BF16)
    go(pair_copy(2))
    own[...] = term(xo, c)
    go(pair_copy(3))
    pair_copy(0).wait_recv()
    far2[...] = (own[...] + from_pair[0].astype(F32)).astype(BF16).reshape(2, 128, TOK)
    own[...] = term(xr, c)
    far_r = remote(far2.at[0], in_far.at[0], rs_send.at[4], rs_recv.at[4], right)
    far_l = remote(far2.at[1], in_far.at[1], rs_send.at[5], rs_recv.at[5], left)
    go(far_r)
    go(far_l)
    pair_copy(1).wait_recv()
    keep_r[...] = own[0:128] + from_pair[1, 0:128].astype(F32)
    rgt[1] = (own[128:256] + from_pair[1, 128:256].astype(F32)).astype(BF16)
    own[...] = term(xl, c)
    r_plain = remote(rgt.at[1], in_l.at[1], rs_send.at[6], rs_recv.at[6], right)
    go(r_plain)
    pair_copy(2).wait_recv()
    keep_l[...] = own[128:256] + from_pair[2, 128:256].astype(F32)
    lft[0] = (own[0:128] + from_pair[2, 0:128].astype(F32)).astype(BF16)
    own[...] = term(x, c)
    l_plain = remote(lft.at[0], in_r.at[0], rs_send.at[7], rs_recv.at[7], left)
    go(l_plain)
    pair_copy(3).wait_recv()
    for a in range(8):
        at = slice(a * 32, (a + 1) * 32)
        own[at] = own[at] + from_pair[3, at].astype(F32) + x1b[tp * 8 + a].astype(F32)
    far_r.wait_recv()
    rgt[0] = (keep_r[...] + in_far[0].astype(F32)).astype(BF16)
    r_sum = remote(rgt.at[0], in_l.at[0], rs_send.at[8], rs_recv.at[8], right)
    go(r_sum)
    far_l.wait_recv()
    lft[1] = (keep_l[...] + in_far[1].astype(F32)).astype(BF16)
    l_sum = remote(lft.at[1], in_r.at[1], rs_send.at[9], rs_recv.at[9], left)
    go(l_sum)
    r_plain.wait_recv()
    l_plain.wait_recv()
    own[128:256] = own[128:256] + in_l[1].astype(F32)
    own[0:128] = own[0:128] + in_r[0].astype(F32)
    r_sum.wait_recv()
    l_sum.wait_recv()
    own[0:128] = own[0:128] + in_l[0].astype(F32)
    own[128:256] = own[128:256] + in_r[1].astype(F32)

    total = jnp.sum(own[...] * own[...], axis=0, keepdims=True)
    ssq[tp] = total

    def q_copy(o, at):
        t = (tp + o) % 8
        return remote(ssq.at[at], ssq.at[at], q_send.at[o - 1], q_recv.at[o - 1], device(z, y, t // 2, t % 2))

    gain3 = jnp.concatenate(
        [wide(spread_row(g3_ref[pl.ds(tp * 2 + i, 1), :]), 4) for i in range(2)], axis=0
    )
    for o in range(1, 8):
        go(q_copy(o, tp))
    for o in range(1, 8):
        q_copy(o, (tp - o + 8) % 8).wait_recv()
    squares = ssq[0]
    for k in range(1, 8):
        squares = squares + ssq[k]
    fac = lax.rsqrt(squares / D + EPS)
    out_ref[...] = (own[...] * fac * gain3).astype(BF16)
    for copy in started:
        copy.wait_send()


def on_device(
    activations, w_mix_in, w_mix_out, w_gate, w_up, w_down, pool_scale, gain_mix, gain_ffn, gain_out
):
    pad = ((0, 0), (0, HID - w_gate.shape[1]))
    wf = jnp.stack([jnp.pad(w, pad) for w in (w_gate, w_up, w_down)])
    vmem = pl.BlockSpec(memory_space=pltpu.VMEM)
    hbm = pl.BlockSpec(memory_space=pl.ANY)
    dma = pltpu.SemaphoreType.DMA
    rows = lambda width: pltpu.VMEM((8, 8, 32, width), BF16)
    return pl.pallas_call(
        kernel,
        out_shape=jax.ShapeDtypeStruct((256, TOK), BF16),
        in_specs=[hbm] * 4 + [vmem] * 4,
        out_specs=vmem,
        scratch_shapes=[
            pltpu.VMEM((64, 32, TOK), BF16),
            pltpu.VMEM((64, 32, TOK), BF16),
            pltpu.VMEM((64, 32, TOK), BF16),
            rows(128), rows(512), rows(512), rows(HID), rows(HID), rows(HID),
            pltpu.VMEM((4, 128, TOK), BF16),
            pltpu.VMEM((4, 128, TOK), BF16),
            pltpu.VMEM((64, 32, 128), F32),
            pltpu.VMEM((HID, TOK), BF16),
            pltpu.VMEM((4, 256, TOK), BF16),
            pltpu.VMEM((4, 256, TOK), BF16),
            pltpu.VMEM((256, TOK), F32),
            pltpu.VMEM((2, 128, TOK), BF16),
            pltpu.VMEM((2, 128, TOK), BF16),
            pltpu.VMEM((2, 128, TOK), BF16),
            pltpu.VMEM((128, TOK), F32),
            pltpu.VMEM((128, TOK), F32),
            pltpu.VMEM((2, 128, TOK), BF16),
            pltpu.VMEM((2, 128, TOK), BF16),
            pltpu.VMEM((2, 128, TOK), BF16),
            pltpu.VMEM((8, 1, TOK), F32),
            dma((6,)),
            dma((5, 7)), dma((5, 7)),
            dma((5, 2, 8)), dma((5, 2, 8)),
            dma((3,)), dma((3,)),
            dma((8,)), dma((8,)),
            dma((8,)), dma((8,)),
            dma((10,)), dma((10,)),
            dma((7,)), dma((7,)),
        ],
        compiler_params=pltpu.CompilerParams(
            collective_id=0, has_side_effects=True, vmem_limit_bytes=60 * 1024 * 1024
        ),
        name="layer",
    )(
        activations.reshape(64, 32, TOK), w_mix_in, w_mix_out, wf,
        pool_scale.reshape(8, 128), gain_mix.reshape(16, 128),
        gain_ffn.reshape(16, 128), gain_out.reshape(16, 128),
    )


def solution(mesh):
    shards = P("fs", "tp")
    placed = (P(None, ("rep", "fs")),) + (shards,) * 5 + (P(),) * 4
    return jax.shard_map(
        on_device, mesh=mesh, in_specs=placed, out_specs=P("tp", ("rep", "fs")), check_vma=False
    )
```

```python
import jax
import jax.numpy as jnp
from jax import lax
from jax.experimental import pallas as pl
from jax.experimental.pallas import tpu as pltpu
from jax.sharding import PartitionSpec as P

F32 = jnp.float32
BF16 = jnp.bfloat16
SEQ = 256
EPS = 1e-06
TOK = 512
D = 2048
HID = 384
MESH = pl.DeviceIdType.MESH
MIX_IN, MIX_OUT, GATE, UP, DOWN = range(5)
HALVES = (1, 1, 2, 2, 2)
CHUNKS = ((0, 1, 7), (2, 6), (3, 4, 5))


def wide(tile, times):
    return jnp.concatenate([tile] * times, axis=1)


def spread_row(row):
    return jnp.transpose(jnp.broadcast_to(row, (128, 128)))


def dot(a, b):
    return jnp.dot(a, b, preferred_element_type=F32)


def dot_first(a, b):
    return lax.dot_general(a, b, (((0,), (0,)), ((), ())), preferred_element_type=F32)


def kernel(
    x_hbm, wi_hbm, wo_hbm, wg_ref, wu_ref, wd_ref, scale_ref, g1_ref, g2_ref, g3_ref,
    out_ref,
    xb, hb, x1b, mb, ob, opb, gb, ub, db, pc, pp, gcol, hid, g_acc, u_acc,
    to_pair, from_pair, own, far2, rgt, lft, keep_r, keep_l, in_l, in_r, in_far, ssq,
    loc_sem, p1_send, p1_recv, p1r_recv, p2_send, p2_recv, xo_send, xo_recv, d2_send, d2_recv,
    p_send, p_recv, rs_send, rs_recv, q_send, q_recv,
):
    rep, fs, tp = lax.axis_index("rep"), lax.axis_index("fs"), lax.axis_index("tp")
    zl, y = fs // 8, fs % 8
    z = rep * 8 + zl
    x, c = tp // 2, tp % 2
    a_own = y + c * (zl - y)
    b_own = zl + c * (y - zl)

    def device(zz, yy, xx, cc):
        zz = (zz + 32) % 16
        yy = (yy + 16) % 8
        return (zz // 8, (zz % 8) * 8 + yy, ((xx + 8) % 4) * 2 + cc)

    def ring_a(d):
        return device(z + c * d, y + (1 - c) * d, x, c)

    def ring_b(d):
        return device(z + (1 - c) * d, y + c * d, x, c)

    def fidx(b, a):
        return (b * 8 + a) + c * ((a * 8 + b) - (b * 8 + a))

    started = []

    def remote(src, dst, send, recv, dev):
        return pltpu.make_async_remote_copy(
            src_ref=src, dst_ref=dst, send_sem=send, recv_sem=recv, device_id=dev, device_id_type=MESH
        )

    def go(copy):
        copy.start()
        started.append(copy)

    def drain(keep):
        for _ in range(len(started) - keep):
            started.pop(0).wait_send()

    def lane(xx):
        return pl.ds(pl.multiple_of(xx * 128, 128), 128)

    bufs = (mb, ob.at[:, :, :, lane(x)], gb, ub, db)

    locals_ = [
        pltpu.make_async_copy(wi_hbm, mb.at[b_own, a_own], loc_sem.at[0]),
        pltpu.make_async_copy(
            wo_hbm, ob.at[b_own, a_own, :, lane(x)], loc_sem.at[1]
        ),
    ]
    x_copy = pltpu.make_async_copy(x_hbm, xb, loc_sem.at[2])
    for cp in locals_:
        cp.start()
    x_copy.start()
    barrier = pltpu.get_barrier_semaphore()
    peers = [ring_a(d) for d in (1, -1, 2, -2, 3, -3, 4, -4)] + [ring_b(1), ring_b(-1)]
    peers += [device(z, y, x + dx, cc) for dx in (1, 2, 3) for cc in (c, 1 - c)]
    peers += [device(z, y, x, 1 - c)]
    for dev in peers:
        pl.semaphore_signal(barrier, inc=1, device_id=dev, device_id_type=MESH)
    for buf, ref in ((gb, wg_ref), (ub, wu_ref), (db, wd_ref)):
        width = ref.shape[1]
        buf[b_own, a_own, :, 0:width] = ref[...]
        buf[b_own, a_own, :, width:HID] = jnp.zeros((32, HID - width), BF16)
    for cp in locals_:
        cp.wait()
    pl.semaphore_wait(barrier, len(peers))

    offsets = (1, -1, 2, -2, 3, -3, 4)

    def p1_start(t):
        blk = bufs[t].at[b_own, a_own]
        for d in offsets:
            remote(blk, blk, p1_send.at[t], p1_recv.at[t], ring_a(d)).start()

    def p1_wait(t):
        blks = bufs[t].at[b_own, pl.ds(0, 7)]
        remote(blks, blks, p1_send.at[t], p1_recv.at[t], ring_a(1)).wait_recv()

    def ring_1(t, d, way, arriving):
        w = (1 - way) // 2
        at = (a_own - way * (d + arriving) + 16) % 8
        blk = bufs[t].at[b_own, at]
        if d == 3:
            blk = bufs[t].at[b_own, at, pl.ds(0 if way == 1 else 16, 16)]
        return remote(blk, blk, p1_send.at[t], p1r_recv.at[t - UP, w * 4 + d], ring_a(way))

    def p1_ring(t, d):
        for way in (1, -1):
            if d:
                ring_1(t, d - 1, way, 1).wait_recv()
            ring_1(t, d, way, 0).start()

    def p1_ring_last(t):
        for way in (1, -1):
            ring_1(t, 3, way, 1).wait_recv()

    p1_start(MIX_IN)
    p1_start(MIX_OUT)
    p1_start(GATE)
    p1_ring(UP, 0)
    p1_ring(DOWN, 0)

    def spread_gain(g_ref):
        for r in range(16):
            gcol[4 * r : 4 * r + 4] = spread_row(g_ref[r : r + 1, :]).reshape(4, 32, 128)

    def add_squares(acc, v):
        return acc + (v * v).reshape(4, 8, TOK).sum(axis=0)

    def factor(acc):
        return lax.rsqrt(jnp.sum(acc, axis=0, keepdims=True) / D + EPS)

    x_copy.wait()
    spread_gain(g1_ref)
    acc1 = lax.fori_loop(
        0, 64, lambda i, acc: add_squares(acc, xb[i].astype(F32)), jnp.zeros((8, TOK), F32)
    )
    r1 = factor(acc1)

    def row_part(t, row, d, way, half):
        if d == 3:
            return bufs[t].at[row, pl.ds(0, 4)] if way == 1 else bufs[t].at[row, pl.ds(4, 4)]
        if HALVES[t] == 2:
            return bufs[t].at[row, pl.ds(4 * half, 4)]
        return bufs[t].at[row]

    def p2(t, d, way, half, arriving):
        w = (1 - way) // 2
        row = (b_own - way * (d + arriving) + 16) % 8
        part = row_part(t, row, d, way, half)
        at = d * 2 + half
        return remote(part, part, p2_send.at[t], p2_recv.at[t, w, at], ring_b(way))

    def parts_of(t, d):
        return range(1 if d == 3 else HALVES[t])

    def forward(t, d, half=0):
        for way in (1, -1):
            if d in (1, 2):
                p2(t, d - 1, way, half, 1).wait_recv()
            elif d == 3:
                own_half = 0 if way == 1 else 1
                if HALVES[t] == 2:
                    p2(t, 2, way, own_half, 1).wait_recv()
                else:
                    p2(t, 2, way, 0, 1).wait_recv()
            p2(t, d, way, half, 0).start()
        if d == 3 and HALVES[t] == 2:
            for way in (1, -1):
                other_half = 1 if way == 1 else 0
                p2(t, 2, way, other_half, 1).wait_recv()

    def last(t):
        for way in (1, -1):
            p2(t, 3, way, 0, 1).wait_recv()

    pair = device(z, y, x, 1 - c)

    xr, xl, xo = (x + 1) % 4, (x + 3) % 4, (x + 2) % 4
    right, left = device(z, y, x + 1, c), device(z, y, x - 1, c)

    def to_pair_row(k):
        row = (b_own - k + 16) % 8
        return remote(ob.at[row], opb.at[:, row], d2_send, d2_recv, pair)

    def x_copy_of(k, chunk, source, way, halved):
        row = (b_own - k + 16) % 8
        part = ob.at[row, :, :, lane(source)]
        if halved:
            part = ob.at[row, pl.ds(0 if way == 1 else 4, 4), :, lane(source)]
        at = (1 - way) // 2 + 2 * halved
        return remote(part, part, xo_send, xo_recv.at[chunk, at], right if way == 1 else left)

    def x_send(k, chunk):
        for way in (1, -1):
            x_copy_of(k, chunk, x, way, 0).start()

    def x_wait(chunk, way, halved):
        rows = pl.ds(0, len(CHUNKS[chunk]))
        part = ob.at[rows, pl.ds(0, 4 if halved else 8), :, pl.ds(0, 128)]
        at = (1 - way) // 2 + 2 * halved
        remote(part, part, xo_send, xo_recv.at[chunk, at], right).wait_recv()

    def x_forward(chunk):
        for way, source in ((1, xl), (-1, xr)):
            x_wait(chunk, way, 0)
            for k in CHUNKS[chunk]:
                x_copy_of(k, chunk, source, way, 1).start()

    def x_last(chunk):
        for way in (1, -1):
            x_wait(chunk, way, 1)
        for k in CHUNKS[chunk]:
            to_pair_row(k).start()

    def scale_h(src, fac):
        def body(i, carry):
            v = src[i].astype(F32) * fac * wide(gcol[i], 4)
            b, a = i // 8, i % 8
            hb[fidx(b, a)] = v.astype(BF16)
            return carry

        lax.fori_loop(0, 64, body, 0)

    def both(t, d):
        forward(t, d, 0)
        forward(t, d, 1)

    scale_h(xb, r1)
    p1_wait(MIX_IN)
    forward(MIX_IN, 0)
    p1_wait(MIX_OUT)
    forward(MIX_OUT, 0)
    x_send(0, 0)
    p1_wait(GATE)
    forward(GATE, 0, 0)
    forward(MIX_IN, 1)
    forward(MIX_OUT, 1)
    x_send(1, 0)
    x_send(7, 0)
    p1_ring(UP, 1)
    p1_ring(DOWN, 1)
    forward(GATE, 0, 1)
    forward(MIX_IN, 2)
    forward(MIX_OUT, 2)
    x_send(2, 1)
    x_send(6, 1)
    p1_ring(UP, 2)
    p1_ring(DOWN, 2)
    forward(GATE, 1, 0)
    forward(MIX_IN, 3)
    forward(MIX_OUT, 3)
    x_forward(0)
    p1_ring(UP, 3)
    p1_ring(DOWN, 3)
    forward(GATE, 1, 1)
    spread_gain(g2_ref)
    last(MIX_IN)

    u = dot_first(mb[...].reshape(D, 128), hb[...].reshape(D, TOK)).astype(BF16)
    behind = lax.shift_left(jnp.int32(1), x.astype(jnp.int32))
    src_place = lax.broadcasted_iota(jnp.int32, (SEQ, SEQ), 0)
    dst_place = lax.broadcasted_iota(jnp.int32, (SEQ, SEQ), 1)
    inside = (src_place >= dst_place - behind) & (src_place < dst_place + behind)
    band = jnp.where(inside, 1.0, 0.0).astype(BF16)
    place = lax.broadcasted_iota(jnp.int32, (1, SEQ), 1)
    counts = (jnp.minimum(place + behind, SEQ) - jnp.maximum(place - behind, 0)).astype(F32)
    scale_col = wide(spread_row(scale_ref[pl.ds(tp, 1), :]), 2)
    for s in range(2):
        us = u[:, s * SEQ : (s + 1) * SEQ]
        mean = dot(us, band) / counts
        pc[x, :, s * SEQ : (s + 1) * SEQ] = ((mean - us.astype(F32)) * scale_col).astype(BF16)

    lo, hi = pl.ds(0, 64), pl.ds(64, 64)
    p_own_r = remote(pc.at[x], pc.at[x], p_send.at[0], p_recv.at[0], right)
    p_own_l = remote(pc.at[x], pc.at[x], p_send.at[1], p_recv.at[1], left)
    go(p_own_r)
    go(p_own_l)
    go(remote(pc.at[x], pp.at[x], p_send.at[2], p_recv.at[2], pair))
    last(MIX_OUT)
    for k in CHUNKS[2]:
        x_send(k, 2)
    p1_ring_last(UP)
    both(UP, 0)
    p1_ring_last(DOWN)
    both(DOWN, 0)
    x_forward(1)
    both(GATE, 2)
    p_own_r.wait_recv()
    go(remote(pc.at[xl, lo], pc.at[xl, lo], p_send.at[3], p_recv.at[3], right))
    go(remote(pc.at[xl], pp.at[xl], p_send.at[4], p_recv.at[4], pair))
    p_own_l.wait_recv()
    go(remote(pc.at[xr, hi], pc.at[xr, hi], p_send.at[5], p_recv.at[5], left))
    go(remote(pc.at[xr], pp.at[xr], p_send.at[6], p_recv.at[6], pair))
    both(UP, 1)
    x_last(0)
    both(DOWN, 1)
    x_forward(2)
    both(UP, 2)
    remote(pc.at[xo, lo], pc.at[xo, lo], p_send.at[3], p_recv.at[3], right).wait_recv()
    remote(pc.at[xo, hi], pc.at[xo, hi], p_send.at[5], p_recv.at[5], left).wait_recv()
    go(remote(pc.at[xo], pp.at[xo], p_send.at[7], p_recv.at[7], pair))
    x_last(1)
    x_last(2)
    both(DOWN, 2)
    for n, at in ((2, x), (4, xl), (6, xr), (7, xo)):
        remote(pc.at[at], pp.at[at], p_send.at[n], p_recv.at[n], pair).wait_recv()
    remote(ob, opb, d2_send, d2_recv, pair).wait_recv()

    def mix_row(b, acc):
        m = dot(ob[b].reshape(256, 512), pc[...].reshape(512, TOK))
        m = m + dot(opb[b].reshape(256, 512), pp[...].reshape(512, TOK))
        for a in range(8):
            f = fidx(b, a)
            v = (xb[f].astype(F32) + m[a * 32 : (a + 1) * 32]).astype(BF16)
            x1b[f] = v
            acc = add_squares(acc, v.astype(F32))
        return acc

    acc2 = lax.fori_loop(0, 4, mix_row, jnp.zeros((8, TOK), F32))
    forward(GATE, 3)
    acc2 = lax.fori_loop(4, 8, mix_row, acc2)
    forward(UP, 3)
    scale_h(x1b, factor(acc2))

    def products(steps, first, final):
        places = [(b_own + k + 8) % 8 for k in steps]

        def half(n, carry):
            at = pl.ds(pl.multiple_of(n * 256, 256), 256)
            sums = []
            for buf, acc in ((gb, g_acc), (ub, u_acc)):
                total = None if first else acc[:, at]
                for r in places:
                    part = dot_first(buf[r].reshape(256, HID), hb[pl.ds(r * 8, 8), :, at].reshape(256, 256))
                    total = part if total is None else total + part
                if not final:
                    acc[:, at] = total
                sums.append(total)
            if final:
                g, v = sums
                hid[:, at] = (g / (1.0 + jnp.exp(-g)) * v).astype(BF16)
            return carry

        lax.fori_loop(0, 2, half, 0)

    products((0, 1, -1), True, False)
    forward(DOWN, 3)
    products((2, -2), False, False)
    products((3, -3), False, False)
    last(GATE)
    last(UP)
    products((4,), False, True)
    last(DOWN)

    def term(xd, cd):
        t = xd * 2 + cd
        rows = [db[t + c * (i - t), i + c * (t - i)] for i in range(8)]
        return dot(jnp.concatenate(rows, axis=0), hid[...])

    def pair_copy(j):
        return remote(to_pair.at[j], from_pair.at[j], rs_send.at[j], rs_recv.at[j], pair)

    dests = (xo, xr, xl, x)
    to_pair[0] = term(xo, 1 - c).astype(BF16)
    to_pair[1] = term(xr, 1 - c).astype(BF16)
    go(pair_copy(0))
    to_pair[2] = term(xl, 1 - c).astype(BF16)
    go(pair_copy(1))
    to_pair[3] = term(x, 1 - c).astype(BF16)
    go(pair_copy(2))
    own[...] = term(xo, c)
    go(pair_copy(3))
    pair_copy(0).wait_recv()
    far2[...] = (own[...] + from_pair[0].astype(F32)).astype(BF16).reshape(2, 128, TOK)
    own[...] = term(xr, c)
    far_r = remote(far2.at[0], in_far.at[0], rs_send.at[4], rs_recv.at[4], right)
    far_l = remote(far2.at[1], in_far.at[1], rs_send.at[5], rs_recv.at[5], left)
    go(far_r)
    go(far_l)
    pair_copy(1).wait_recv()
    keep_r[...] = own[0:128] + from_pair[1, 0:128].astype(F32)
    rgt[1] = (own[128:256] + from_pair[1, 128:256].astype(F32)).astype(BF16)
    own[...] = term(xl, c)
    r_plain = remote(rgt.at[1], in_l.at[1], rs_send.at[6], rs_recv.at[6], right)
    go(r_plain)
    pair_copy(2).wait_recv()
    keep_l[...] = own[128:256] + from_pair[2, 128:256].astype(F32)
    lft[0] = (own[0:128] + from_pair[2, 0:128].astype(F32)).astype(BF16)
    own[...] = term(x, c)
    l_plain = remote(lft.at[0], in_r.at[0], rs_send.at[7], rs_recv.at[7], left)
    go(l_plain)
    pair_copy(3).wait_recv()
    for a in range(8):
        at = slice(a * 32, (a + 1) * 32)
        own[at] = own[at] + from_pair[3, at].astype(F32) + x1b[tp * 8 + a].astype(F32)
    for t in range(5):
        seven = bufs[t].at[0, pl.ds(0, 7)]
        remote(seven, seven, p1_send.at[t], p1_send.at[t], pair).wait_send()
        rows = bufs[t].at[pl.ds(0, 7)]
        remote(rows, rows, p2_send.at[t], p2_send.at[t], pair).wait_send()
    sent = ob.at[pl.ds(0, 6)]
    remote(sent, sent, xo_send, xo_send, pair).wait_send()
    remote(ob, opb, d2_send, d2_recv, pair).wait_send()
    drain(4)
    far_r.wait_recv()
    rgt[0] = (keep_r[...] + in_far[0].astype(F32)).astype(BF16)
    r_sum = remote(rgt.at[0], in_l.at[0], rs_send.at[8], rs_recv.at[8], right)
    go(r_sum)
    far_l.wait_recv()
    lft[1] = (keep_l[...] + in_far[1].astype(F32)).astype(BF16)
    l_sum = remote(lft.at[1], in_r.at[1], rs_send.at[9], rs_recv.at[9], left)
    go(l_sum)
    r_plain.wait_recv()
    l_plain.wait_recv()
    own[128:256] = own[128:256] + in_l[1].astype(F32)
    own[0:128] = own[0:128] + in_r[0].astype(F32)
    r_sum.wait_recv()
    l_sum.wait_recv()
    own[0:128] = own[0:128] + in_l[0].astype(F32)
    own[128:256] = own[128:256] + in_r[1].astype(F32)

    total = jnp.sum(own[...] * own[...], axis=0, keepdims=True)
    ssq[tp] = total

    gain3 = jnp.concatenate(
        [wide(spread_row(g3_ref[pl.ds(tp * 2 + i, 1), :]), 4) for i in range(2)], axis=0
    )
    for o in range(1, 8):
        t = (tp + o) % 8
        remote(ssq.at[tp], ssq.at[tp], q_send, q_recv, device(z, y, t // 2, t % 2)).start()
    seven = ssq.at[pl.ds(0, 7)]
    squares_copy = remote(seven, seven, q_send, q_recv, pair)
    squares_copy.wait_recv()
    squares = ssq[0]
    for k in range(1, 8):
        squares = squares + ssq[k]
    fac = lax.rsqrt(squares / D + EPS)
    out_ref[...] = (own[...] * fac * gain3).astype(BF16)
    squares_copy.wait_send()
    drain(0)


def on_device(
    activations, w_mix_in, w_mix_out, w_gate, w_up, w_down, pool_scale, gain_mix, gain_ffn, gain_out
):
    vmem = pl.BlockSpec(memory_space=pltpu.VMEM)
    hbm = pl.BlockSpec(memory_space=pl.ANY)
    dma = pltpu.SemaphoreType.DMA
    rows = lambda width: pltpu.VMEM((8, 8, 32, width), BF16)
    return pl.pallas_call(
        kernel,
        out_shape=jax.ShapeDtypeStruct((256, TOK), BF16),
        in_specs=[hbm] * 3 + [vmem] * 7,
        out_specs=vmem,
        scratch_shapes=[
            pltpu.VMEM((64, 32, TOK), BF16),
            pltpu.VMEM((64, 32, TOK), BF16),
            pltpu.VMEM((64, 32, TOK), BF16),
            rows(128), rows(512), rows(512), rows(HID), rows(HID), rows(HID),
            pltpu.VMEM((4, 128, TOK), BF16),
            pltpu.VMEM((4, 128, TOK), BF16),
            pltpu.VMEM((64, 32, 128), F32),
            pltpu.VMEM((HID, TOK), BF16),
            pltpu.VMEM((HID, TOK), F32),
            pltpu.VMEM((HID, TOK), F32),
            pltpu.VMEM((4, 256, TOK), BF16),
            pltpu.VMEM((4, 256, TOK), BF16),
            pltpu.VMEM((256, TOK), F32),
            pltpu.VMEM((2, 128, TOK), BF16),
            pltpu.VMEM((2, 128, TOK), BF16),
            pltpu.VMEM((2, 128, TOK), BF16),
            pltpu.VMEM((128, TOK), F32),
            pltpu.VMEM((128, TOK), F32),
            pltpu.VMEM((2, 128, TOK), BF16),
            pltpu.VMEM((2, 128, TOK), BF16),
            pltpu.VMEM((2, 128, TOK), BF16),
            pltpu.VMEM((8, 1, TOK), F32),
            dma((3,)),
            dma((5,)), dma((3,)), dma((2, 8)),
            dma((5,)), dma((5, 2, 8)),
            dma, dma((3, 4)),
            dma, dma,
            dma((8,)), dma((8,)),
            dma((10,)), dma((10,)),
            dma, dma,
        ],
        compiler_params=pltpu.CompilerParams(
            collective_id=0, has_side_effects=True, vmem_limit_bytes=60 * 1024 * 1024
        ),
        name="layer",
    )(
        activations.reshape(64, 32, TOK), w_mix_in, w_mix_out, w_gate, w_up, w_down,
        pool_scale.reshape(8, 128), gain_mix.reshape(16, 128),
        gain_ffn.reshape(16, 128), gain_out.reshape(16, 128),
    )


def solution(mesh):
    shards = P("fs", "tp")
    placed = (P(None, ("rep", "fs")),) + (shards,) * 5 + (P(),) * 4
    return jax.shard_map(
        on_device, mesh=mesh, in_specs=placed, out_specs=P("tp", ("rep", "fs")), check_vma=False
    )
```

```python
import jax
import jax.numpy as jnp
from jax import lax
from jax.experimental import pallas as pl
from jax.experimental.pallas import tpu as pltpu
from jax.sharding import PartitionSpec as P

F32 = jnp.float32
BF16 = jnp.bfloat16
SEQ = 256
EPS = 1e-06
TOK = 512
D = 2048
HID = 384
MESH = pl.DeviceIdType.MESH
MIX_IN, MIX_OUT, GATE, UP, DOWN = range(5)
HALVES = (1, 1, 2, 2, 2)
CHUNKS = ((0, 1, 7), (2, 6), (3, 4, 5))


def wide(tile, times):
    return jnp.concatenate([tile] * times, axis=1)


def spread_row(row):
    return jnp.transpose(jnp.broadcast_to(row, (128, 128)))


def dot(a, b):
    return jnp.dot(a, b, preferred_element_type=F32)


def dot_first(a, b):
    return lax.dot_general(a, b, (((0,), (0,)), ((), ())), preferred_element_type=F32)


def kernel(
    x_hbm, wi_hbm, wo_hbm, wg_hbm, wu_hbm, wd_hbm, scale_hbm, g1_hbm, g2_hbm, g3_hbm,
    out_ref,
    xb, hb, x1b, mb, ob, opb, gb, ub, db, pc, pp, gcol, hid, g_acc, u_acc, mix1, w_in, scale_ref, g1_ref, g2_ref, g3_ref,
    to_pair, from_pair, own, far2, rgt, lft, keep_r, keep_l, in_l, in_r, in_far, ssq,
    loc_sem, p1_send, p1_recv, p1r_recv, p2_send, mo_recv, p2_recv, xo_send, xo_recv, d2_send, d2_recv,
    p_send, p_recv, rs_send, rs_recv, q_send, q_recv,
):
    rep, fs, tp = lax.axis_index("rep"), lax.axis_index("fs"), lax.axis_index("tp")
    zl, y = fs // 8, fs % 8
    z = rep * 8 + zl
    x, c = tp // 2, tp % 2
    a_own = y + c * (zl - y)
    b_own = zl + c * (y - zl)

    def device(zz, yy, xx, cc):
        zz = (zz + 32) % 16
        yy = (yy + 16) % 8
        return (zz // 8, (zz % 8) * 8 + yy, ((xx + 8) % 4) * 2 + cc)

    def ring_a(d):
        return device(z + c * d, y + (1 - c) * d, x, c)

    def ring_b(d):
        return device(z + (1 - c) * d, y + c * d, x, c)

    def fidx(b, a):
        return (b * 8 + a) + c * ((a * 8 + b) - (b * 8 + a))

    started = []

    def remote(src, dst, send, recv, dev):
        return pltpu.make_async_remote_copy(
            src_ref=src, dst_ref=dst, send_sem=send, recv_sem=recv, device_id=dev, device_id_type=MESH
        )

    def go(copy):
        copy.start()
        started.append(copy)

    def drain(keep):
        for _ in range(len(started) - keep):
            started.pop(0).wait_send()

    def lane(xx):
        return pl.ds(pl.multiple_of(xx * 128, 128), 128)

    bufs = (mb, ob.at[:, :, :, lane(x)], gb, ub, db)

    locals_ = [
        pltpu.make_async_copy(wi_hbm, mb.at[b_own, a_own], loc_sem.at[0]),
        pltpu.make_async_copy(
            wo_hbm, ob.at[b_own, a_own, :, lane(x)], loc_sem.at[1]
        ),
    ]
    x_copy = pltpu.make_async_copy(x_hbm, xb, loc_sem.at[2])
    w_copies = [
        pltpu.make_async_copy(src, w_in.at[i], loc_sem.at[3 + i])
        for i, src in enumerate((wg_hbm, wu_hbm, wd_hbm))
    ]
    small = [
        pltpu.make_async_copy(src, dst, loc_sem.at[6 + i])
        for i, (src, dst) in enumerate(
            ((g1_hbm, g1_ref), (g2_hbm, g2_ref), (g3_hbm, g3_ref), (scale_hbm, scale_ref))
        )
    ]
    for cp in locals_ + w_copies + small:
        cp.start()
    x_copy.start()
    barrier = pltpu.get_barrier_semaphore()
    peers = [ring_a(d) for d in (1, -1, 2, -2, 3, -3, 4, -4)] + [ring_b(1), ring_b(-1), ring_b(2), ring_b(-2)]
    peers += [device(z, y, x + dx, cc) for dx in (1, 2, 3) for cc in (c, 1 - c)]
    peers += [device(z, y, x, 1 - c)]
    for dev in peers:
        pl.semaphore_signal(barrier, inc=1, device_id=dev, device_id_type=MESH)
    for cp in w_copies:
        cp.wait()
    width = w_in.shape[2]
    for i, buf in enumerate((gb, ub, db)):
        buf[b_own, a_own, :, 0:width] = w_in[i]
        buf[b_own, a_own, :, width:HID] = jnp.zeros((32, HID - width), BF16)
    for cp in locals_:
        cp.wait()
    pl.semaphore_wait(barrier, len(peers))

    offsets = (1, -1, 2, -2, 3, -3, 4)

    def p1_start(t):
        blk = bufs[t].at[b_own, a_own]
        for d in offsets:
            remote(blk, blk, p1_send.at[t], p1_recv.at[t], ring_a(d)).start()

    def p1_wait(t):
        blks = bufs[t].at[b_own, pl.ds(0, 7)]
        remote(blks, blks, p1_send.at[t], p1_recv.at[t], ring_a(1)).wait_recv()

    def ring_1(t, d, way):
        at = (a_own - way * d + 16) % 8
        blk = bufs[t].at[b_own, at]
        if d == 3:
            blk = bufs[t].at[b_own, at, pl.ds(0 if way == 1 else 16, 16)]
        return remote(blk, blk, p1_send.at[t], p1r_recv.at[(1 - way) * 2 + d], ring_a(way))

    def ring_1_wait(d, way):
        both_types = ub.at[b_own, pl.ds(0, 2)] if d < 3 else ub.at[b_own, 0]
        sem = p1r_recv.at[(1 - way) * 2 + d]
        remote(both_types, both_types, p1_send.at[UP], sem, ring_a(way)).wait_recv()

    def p1_ring(d):
        for way in (1, -1):
            if d:
                ring_1_wait(d - 1, way)
            for t in (UP, DOWN):
                ring_1(t, d, way).start()

    def p1_ring_last():
        for way in (1, -1):
            ring_1_wait(3, way)

    p1_start(MIX_IN)
    p1_start(MIX_OUT)
    p1_start(GATE)
    p1_ring(0)

    def spread_gain(g_ref):
        for r in range(16):
            gcol[4 * r : 4 * r + 4] = spread_row(g_ref[r : r + 1, :]).reshape(4, 32, 128)

    def add_squares(acc, v):
        return acc + (v * v).reshape(4, 8, TOK).sum(axis=0)

    def factor(acc):
        return lax.rsqrt(jnp.sum(acc, axis=0, keepdims=True) / D + EPS)

    x_copy.wait()
    for cp in small:
        cp.wait()
    spread_gain(g1_ref)
    acc1 = lax.fori_loop(
        0, 64, lambda i, acc: add_squares(acc, xb[i].astype(F32)), jnp.zeros((8, TOK), F32)
    )
    r1 = factor(acc1)

    def row_part(t, row, d, way, half):
        if d == 3:
            return bufs[t].at[row, pl.ds(0, 4)] if way == 1 else bufs[t].at[row, pl.ds(4, 4)]
        if HALVES[t] == 2:
            return bufs[t].at[row, pl.ds(4 * half, 4)]
        return bufs[t].at[row]

    def p2(t, d, way, half, arriving):
        w = (1 - way) // 2
        row = (b_own - way * (d + arriving) + 16) % 8
        part = row_part(t, row, d, way, half)
        at = d * 2 + half
        return remote(part, part, p2_send.at[t], p2_recv.at[t - GATE, w, at], ring_b(way))

    def parts_of(t, d):
        return range(1 if d == 3 else HALVES[t])

    def forward(t, d, half=0):
        for way in (1, -1):
            if d in (1, 2):
                p2(t, d - 1, way, half, 1).wait_recv()
            elif d == 3:
                own_half = 0 if way == 1 else 1
                if HALVES[t] == 2:
                    p2(t, 2, way, own_half, 1).wait_recv()
                else:
                    p2(t, 2, way, 0, 1).wait_recv()
            p2(t, d, way, half, 0).start()
        if d == 3 and HALVES[t] == 2:
            for way in (1, -1):
                other_half = 1 if way == 1 else 0
                p2(t, 2, way, other_half, 1).wait_recv()

    def last(t):
        for way in (1, -1):
            p2(t, 3, way, 0, 1).wait_recv()

    def jump(t, step, way, arriving):
        w = (1 - way) // 2
        hops = (1, 2, 1, 2)[step]
        held = (0, 0, 2, 2)[step]
        row = (b_own - way * (held + hops * arriving) + 16) % 8
        part = bufs[t].at[row]
        if step == 3:
            part = bufs[t].at[row, pl.ds(0 if way == 1 else 4, 4)]
        return remote(part, part, p2_send.at[t], mo_recv.at[t, w, step], ring_b(way * hops))

    def jump_start(t):
        for step in (1, 0):
            for way in (1, -1):
                jump(t, step, way, 0).start()

    def jump_wait(t, step):
        for way in (1, -1):
            jump(t, step, way, 1).wait_recv()

    def jump_on(t):
        for way in (1, -1):
            jump(t, 1, way, 1).wait_recv()
            jump(t, 3, way, 0).start()
            jump(t, 2, way, 0).start()

    pair = device(z, y, x, 1 - c)

    xr, xl, xo = (x + 1) % 4, (x + 3) % 4, (x + 2) % 4
    right, left = device(z, y, x + 1, c), device(z, y, x - 1, c)

    def pair_part(k, source):
        row = (b_own - k + 16) % 8
        src, dst = ob.at[row, :, :, lane(source)], opb.at[:, row, :, lane(source)]
        remote(src, dst, d2_send, d2_recv, pair).start()

    def x_copy_of(k, chunk, source, way, halved):
        row = (b_own - k + 16) % 8
        part = ob.at[row, :, :, lane(source)]
        if halved:
            part = ob.at[row, pl.ds(0 if way == 1 else 4, 4), :, lane(source)]
        at = (1 - way) // 2 + 2 * halved
        return remote(part, part, xo_send, xo_recv.at[chunk, at], right if way == 1 else left)

    def x_send(k, chunk):
        for way in (1, -1):
            x_copy_of(k, chunk, x, way, 0).start()
        pair_part(k, x)

    def x_wait(chunk, way, halved):
        rows = pl.ds(0, len(CHUNKS[chunk]))
        part = ob.at[rows, pl.ds(0, 4 if halved else 8), :, pl.ds(0, 128)]
        at = (1 - way) // 2 + 2 * halved
        remote(part, part, xo_send, xo_recv.at[chunk, at], right).wait_recv()

    def x_forward(chunk):
        for way, source in ((1, xl), (-1, xr)):
            x_wait(chunk, way, 0)
            for k in CHUNKS[chunk]:
                x_copy_of(k, chunk, source, way, 1).start()
            for k in CHUNKS[chunk]:
                pair_part(k, source)

    def x_last(chunk):
        for way in (1, -1):
            x_wait(chunk, way, 1)
        for k in CHUNKS[chunk]:
            pair_part(k, xo)

    def scale_h(src, fac):
        def body(i, carry):
            v = src[i].astype(F32) * fac * wide(gcol[i], 4)
            b, a = i // 8, i % 8
            hb[fidx(b, a)] = v.astype(BF16)
            return carry

        lax.fori_loop(0, 64, body, 0)

    def both(t, d):
        forward(t, d, 0)
        forward(t, d, 1)

    scale_h(xb, r1)
    p1_wait(MIX_IN)
    jump_start(MIX_IN)
    p1_wait(MIX_OUT)
    jump_start(MIX_OUT)
    x_send(0, 0)
    p1_wait(GATE)
    forward(GATE, 0, 0)
    p1_ring(1)
    jump_on(MIX_IN)
    jump_on(MIX_OUT)
    x_send(2, 1)
    x_send(6, 1)
    jump_wait(MIX_OUT, 0)
    x_send(1, 0)
    x_send(7, 0)
    forward(GATE, 0, 1)
    p1_ring(2)
    forward(GATE, 1, 0)
    spread_gain(g2_ref)
    jump_wait(MIX_IN, 0)
    jump_wait(MIX_IN, 2)
    jump_wait(MIX_IN, 3)

    u = dot_first(mb[...].reshape(D, 128), hb[...].reshape(D, TOK)).astype(BF16)
    behind = lax.shift_left(jnp.int32(1), x.astype(jnp.int32))
    src_place = lax.broadcasted_iota(jnp.int32, (SEQ, SEQ), 0)
    dst_place = lax.broadcasted_iota(jnp.int32, (SEQ, SEQ), 1)
    inside = (src_place >= dst_place - behind) & (src_place < dst_place + behind)
    band = jnp.where(inside, 1.0, 0.0).astype(BF16)
    place = lax.broadcasted_iota(jnp.int32, (1, SEQ), 1)
    counts = (jnp.minimum(place + behind, SEQ) - jnp.maximum(place - behind, 0)).astype(F32)
    scale_col = wide(spread_row(scale_ref[pl.ds(tp, 1), :]), 2)
    for s in range(2):
        us = u[:, s * SEQ : (s + 1) * SEQ]
        mean = dot(us, band) / counts
        pc[x, :, s * SEQ : (s + 1) * SEQ] = ((mean - us.astype(F32)) * scale_col).astype(BF16)

    lo, hi = pl.ds(0, 64), pl.ds(64, 64)
    p_own_r = remote(pc.at[x], pc.at[x], p_send.at[0], p_recv.at[0], right)
    p_own_l = remote(pc.at[x], pc.at[x], p_send.at[1], p_recv.at[1], left)
    go(p_own_r)
    go(p_own_l)
    go(remote(pc.at[x], pp.at[x], p_send.at[2], p_recv.at[2], pair))
    jump_wait(MIX_OUT, 2)
    jump_wait(MIX_OUT, 3)
    for k in CHUNKS[2]:
        x_send(k, 2)
    p1_ring(3)
    forward(GATE, 1, 1)
    x_forward(0)
    p1_ring_last()
    both(UP, 0)
    both(DOWN, 0)
    x_forward(1)
    both(GATE, 2)
    p_own_r.wait_recv()
    go(remote(pc.at[xl, lo], pc.at[xl, lo], p_send.at[3], p_recv.at[3], right))
    go(remote(pc.at[xl], pp.at[xl], p_send.at[4], p_recv.at[4], pair))
    p_own_l.wait_recv()
    go(remote(pc.at[xr, hi], pc.at[xr, hi], p_send.at[5], p_recv.at[5], left))
    go(remote(pc.at[xr], pp.at[xr], p_send.at[6], p_recv.at[6], pair))
    both(UP, 1)
    x_last(0)
    both(DOWN, 1)
    x_forward(2)
    x_last(1)
    both(UP, 2)
    remote(pc.at[xo, lo], pc.at[xo, lo], p_send.at[3], p_recv.at[3], right).wait_recv()
    remote(pc.at[xo, hi], pc.at[xo, hi], p_send.at[5], p_recv.at[5], left).wait_recv()
    go(remote(pc.at[xo], pp.at[xo], p_send.at[7], p_recv.at[7], pair))

    def mix_own(i, carry):
        row = (b_own + 6 + i) % 8
        mix1[row] = dot(ob[row].reshape(256, 512), pc[...].reshape(512, TOK))
        return carry

    lax.fori_loop(0, 5, mix_own, 0)
    x_last(2)
    both(DOWN, 2)
    lax.fori_loop(5, 8, mix_own, 0)
    for n, at in ((2, x), (4, xl), (6, xr), (7, xo)):
        remote(pc.at[at], pp.at[at], p_send.at[n], p_recv.at[n], pair).wait_recv()
    remote(ob, opb, d2_send, d2_recv, pair).wait_recv()

    def mix_row(b, acc):
        m = mix1[b] + dot(opb[b].reshape(256, 512), pp[...].reshape(512, TOK))
        for a in range(8):
            f = fidx(b, a)
            v = (xb[f].astype(F32) + m[a * 32 : (a + 1) * 32]).astype(BF16)
            x1b[f] = v
            acc = add_squares(acc, v.astype(F32))
        return acc

    forward(GATE, 3)
    forward(UP, 3)
    acc2 = lax.fori_loop(0, 4, mix_row, jnp.zeros((8, TOK), F32))
    forward(DOWN, 3)
    acc2 = lax.fori_loop(4, 8, mix_row, acc2)
    scale_h(x1b, factor(acc2))

    def products(steps, first, final):
        places = [(b_own + k + 8) % 8 for k in steps]

        def half(n, carry):
            at = pl.ds(pl.multiple_of(n * 256, 256), 256)
            sums = []
            for buf, acc in ((gb, g_acc), (ub, u_acc)):
                total = None if first else acc[:, at]
                for r in places:
                    part = dot_first(buf[r].reshape(256, HID), hb[pl.ds(r * 8, 8), :, at].reshape(256, 256))
                    total = part if total is None else total + part
                if not final:
                    acc[:, at] = total
                sums.append(total)
            if final:
                g, v = sums
                hid[:, at] = (g / (1.0 + jnp.exp(-g)) * v).astype(BF16)
            return carry

        lax.fori_loop(0, 2, half, 0)

    products((0, 1, -1, 2, -2, 3, -3), True, False)
    last(GATE)
    last(UP)
    products((4,), False, True)
    last(DOWN)

    def term(xd, cd):
        t = xd * 2 + cd
        rows = [db[t + c * (i - t), i + c * (t - i)] for i in range(8)]
        return dot(jnp.concatenate(rows, axis=0), hid[...])

    def pair_copy(j):
        return remote(to_pair.at[j], from_pair.at[j], rs_send.at[j], rs_recv.at[j], pair)

    dests = (xo, xr, xl, x)
    to_pair[0] = term(xo, 1 - c).astype(BF16)
    to_pair[1] = term(xr, 1 - c).astype(BF16)
    go(pair_copy(0))
    to_pair[2] = term(xl, 1 - c).astype(BF16)
    go(pair_copy(1))
    to_pair[3] = term(x, 1 - c).astype(BF16)
    go(pair_copy(2))
    own[...] = term(xo, c)
    go(pair_copy(3))
    pair_copy(0).wait_recv()
    far2[...] = (own[...] + from_pair[0].astype(F32)).astype(BF16).reshape(2, 128, TOK)
    own[...] = term(xr, c)
    far_r = remote(far2.at[0], in_far.at[0], rs_send.at[4], rs_recv.at[4], right)
    far_l = remote(far2.at[1], in_far.at[1], rs_send.at[5], rs_recv.at[5], left)
    go(far_r)
    go(far_l)
    pair_copy(1).wait_recv()
    keep_r[...] = own[0:128] + from_pair[1, 0:128].astype(F32)
    rgt[1] = (own[128:256] + from_pair[1, 128:256].astype(F32)).astype(BF16)
    own[...] = term(xl, c)
    r_plain = remote(rgt.at[1], in_l.at[1], rs_send.at[6], rs_recv.at[6], right)
    go(r_plain)
    pair_copy(2).wait_recv()
    keep_l[...] = own[128:256] + from_pair[2, 128:256].astype(F32)
    lft[0] = (own[0:128] + from_pair[2, 0:128].astype(F32)).astype(BF16)
    own[...] = term(x, c)
    l_plain = remote(lft.at[0], in_r.at[0], rs_send.at[7], rs_recv.at[7], left)
    go(l_plain)
    pair_copy(3).wait_recv()
    for a in range(8):
        at = slice(a * 32, (a + 1) * 32)
        own[at] = own[at] + from_pair[3, at].astype(F32) + x1b[tp * 8 + a].astype(F32)
    for t in range(5):
        seven = bufs[t].at[0, pl.ds(0, 7)]
        remote(seven, seven, p1_send.at[t], p1_send.at[t], pair).wait_send()
        rows = bufs[t].at[pl.ds(0, 7)]
        remote(rows, rows, p2_send.at[t], p2_send.at[t], pair).wait_send()
    sent = ob.at[pl.ds(0, 6)]
    remote(sent, sent, xo_send, xo_send, pair).wait_send()
    remote(ob, opb, d2_send, d2_recv, pair).wait_send()
    drain(4)
    far_r.wait_recv()
    rgt[0] = (keep_r[...] + in_far[0].astype(F32)).astype(BF16)
    r_sum = remote(rgt.at[0], in_l.at[0], rs_send.at[8], rs_recv.at[8], right)
    go(r_sum)
    far_l.wait_recv()
    lft[1] = (keep_l[...] + in_far[1].astype(F32)).astype(BF16)
    l_sum = remote(lft.at[1], in_r.at[1], rs_send.at[9], rs_recv.at[9], left)
    go(l_sum)
    r_plain.wait_recv()
    l_plain.wait_recv()
    own[128:256] = own[128:256] + in_l[1].astype(F32)
    own[0:128] = own[0:128] + in_r[0].astype(F32)
    r_sum.wait_recv()
    l_sum.wait_recv()
    own[0:128] = own[0:128] + in_l[0].astype(F32)
    own[128:256] = own[128:256] + in_r[1].astype(F32)

    total = jnp.sum(own[...] * own[...], axis=0, keepdims=True)
    ssq[tp] = total

    gain3 = jnp.concatenate(
        [wide(spread_row(g3_ref[pl.ds(tp * 2 + i, 1), :]), 4) for i in range(2)], axis=0
    )
    for o in range(1, 8):
        t = (tp + o) % 8
        remote(ssq.at[tp], ssq.at[tp], q_send, q_recv, device(z, y, t // 2, t % 2)).start()
    seven = ssq.at[pl.ds(0, 7)]
    squares_copy = remote(seven, seven, q_send, q_recv, pair)
    squares_copy.wait_recv()
    squares = ssq[0]
    for k in range(1, 8):
        squares = squares + ssq[k]
    fac = lax.rsqrt(squares / D + EPS)
    out_ref[...] = (own[...] * fac * gain3).astype(BF16)
    squares_copy.wait_send()
    drain(0)


def on_device(
    activations, w_mix_in, w_mix_out, w_gate, w_up, w_down, pool_scale, gain_mix, gain_ffn, gain_out
):
    vmem = pl.BlockSpec(memory_space=pltpu.VMEM)
    hbm = pl.BlockSpec(memory_space=pl.ANY)
    dma = pltpu.SemaphoreType.DMA
    rows = lambda width: pltpu.VMEM((8, 8, 32, width), BF16)
    return pl.pallas_call(
        kernel,
        out_shape=jax.ShapeDtypeStruct((256, TOK), BF16),
        in_specs=[hbm] * 10,
        out_specs=vmem,
        scratch_shapes=[
            pltpu.VMEM((64, 32, TOK), BF16),
            pltpu.VMEM((64, 32, TOK), BF16),
            pltpu.VMEM((64, 32, TOK), BF16),
            rows(128), rows(512), rows(512), rows(HID), rows(HID), rows(HID),
            pltpu.VMEM((4, 128, TOK), BF16),
            pltpu.VMEM((4, 128, TOK), BF16),
            pltpu.VMEM((64, 32, 128), F32),
            pltpu.VMEM((HID, TOK), BF16),
            pltpu.VMEM((HID, TOK), F32),
            pltpu.VMEM((HID, TOK), F32),
            pltpu.VMEM((8, 256, TOK), F32),
            pltpu.VMEM((3, *w_gate.shape), BF16),
            pltpu.VMEM((8, 128), F32),
            pltpu.VMEM((16, 128), F32),
            pltpu.VMEM((16, 128), F32),
            pltpu.VMEM((16, 128), F32),
            pltpu.VMEM((4, 256, TOK), BF16),
            pltpu.VMEM((4, 256, TOK), BF16),
            pltpu.VMEM((256, TOK), F32),
            pltpu.VMEM((2, 128, TOK), BF16),
            pltpu.VMEM((2, 128, TOK), BF16),
            pltpu.VMEM((2, 128, TOK), BF16),
            pltpu.VMEM((128, TOK), F32),
            pltpu.VMEM((128, TOK), F32),
            pltpu.VMEM((2, 128, TOK), BF16),
            pltpu.VMEM((2, 128, TOK), BF16),
            pltpu.VMEM((2, 128, TOK), BF16),
            pltpu.VMEM((8, 1, TOK), F32),
            dma((10,)),
            dma((5,)), dma((3,)), dma((8,)),
            dma((5,)), dma((2, 2, 4)), dma((3, 2, 7)),
            dma, dma((3, 4)),
            dma, dma,
            dma((8,)), dma((8,)),
            dma((10,)), dma((10,)),
            dma, dma,
        ],
        compiler_params=pltpu.CompilerParams(
            collective_id=0, has_side_effects=True, vmem_limit_bytes=60 * 1024 * 1024
        ),
        name="layer",
    )(
        activations.reshape(64, 32, TOK), w_mix_in, w_mix_out, w_gate, w_up, w_down,
        pool_scale.reshape(8, 128), gain_mix.reshape(16, 128),
        gain_ffn.reshape(16, 128), gain_out.reshape(16, 128),
    )


def solution(mesh):
    shards = P("fs", "tp")
    placed = (P(None, ("rep", "fs")),) + (shards,) * 5 + (P(),) * 4
    return jax.shard_map(
        on_device, mesh=mesh, in_specs=placed, out_specs=P("tp", ("rep", "fs")), check_vma=False
    )
```
